32 devices in a mesh: sp: 8 (over z, core), tp: 4 (over y, x).
Axes of the slice: x: 2, y: 2, z: 4, core: 2. Of those that a mesh axis runs over, the one named last changes fastest.
Arguments:
- moe_in: bfloat16 [1536, 2048], P('sp'), may hold values from -6 to 6
- cotangent: bfloat16 [1536, 2048], P('sp'), may hold values from -6 to 6
- routing: int32 [1536, 2], P('sp'), may hold values from 0 to 7, as said below
- route_weight: float32 [1536, 2], P('sp'), may hold values from 0.2 to 1
- w_gate: bfloat16 [8, 2048, 2048], P('sp', 'tp'), may hold values from -0.125 to 0.125
- w_up: bfloat16 [8, 2048, 2048], P('sp', 'tp'), may hold values from -0.125 to 0.125
- w_down: bfloat16 [8, 2048, 2048], P('sp', 'tp'), may hold values from -0.125 to 0.125
- gate_b: bfloat16 [1024, 1536], P('tp', 'sp'), may hold values from -6 to 6
- gate_c: bfloat16 [1024, 1536], P('tp', 'sp'), may hold values from -6 to 6
- value_x: bfloat16 [1024, 1536], P('tp', 'sp'), may hold values from -6 to 6
- conv_taps: float32 [3, 1024], P(None, 'tp'), may hold values from -3 to 3
- out_proj: bfloat16 [1024, 2048], P('tp'), may hold values from -0.1875 to 0.1875
Outputs:
- w_gate_grad: bfloat16 [8, 2048, 2048], P('sp', 'tp')
- w_up_grad: bfloat16 [8, 2048, 2048], P('sp', 'tp')
- w_down_grad: bfloat16 [8, 2048, 2048], P('sp', 'tp')
- moe_in_grad: bfloat16 [1536, 2048], P('sp', 'tp')
- proj_grad: float32 [1024, 2048], P('tp', 'sp')
- gate_b_grad: bfloat16 [1024, 1536], P('tp', 'sp')
- gate_c_grad: bfloat16 [1024, 1536], P('tp', 'sp')
- value_x_grad: bfloat16 [1024, 1536], P('tp', 'sp')
The draws below stay inside these ranges and needn't reach their ends.
Inputs may be any that keep to these rules, and one draw needn't show every extreme that they name: `routing`: in each aligned block of 192 rows every expert is named exactly 48 times. The two entries of a row are different experts of one group; group g holds experts g * 2 to g * 2 + 1.
All inputs are finite; a program needn't handle non-finite values.
Results may differ from the reference program's by a relative error of at most 0.025.
Values may be sent and summed in bfloat16 or wider, within the bound.
A program may use at most 64 MiB of HBM per device.

```python
import jax
import jax.numpy as jnp
from jax import lax

D = 2048
W_A = 1024
HID = 2048
TAPS = 3
GROUPS = 4
TOPK = 2
TOK_DEV = 192
TOKENS = 1536
EXPERTS = 8
CAP = 48
HID_DEV = 512
N_SP = 8
N_TP = 4


def route_block(block_key):
    per_group = EXPERTS // GROUPS
    key_rank, key_shift, key_group, key_local = jax.random.split(block_key, 4)
    rank = jax.random.permutation(key_rank, TOK_DEV).astype(jnp.int32)
    first = rank % EXPERTS
    cycle = rank // EXPERTS
    offset = jax.random.randint(key_shift, (), 0, per_group, dtype=jnp.int32)
    shift = (cycle + offset) % max(per_group - 1, 1)
    group_id = first // per_group
    local_one = first % per_group
    local_two = (local_one + 1 + shift) % per_group
    group_perm = jax.random.permutation(key_group, GROUPS).astype(jnp.int32)
    local_perm = jax.random.permutation(key_local, per_group).astype(jnp.int32)
    expert_one = group_perm[group_id] * per_group + local_perm[local_one]
    expert_two = group_perm[group_id] * per_group + local_perm[local_two]
    return jnp.stack([expert_one, expert_two], axis=1)


def draw_routing(key, part):
    block_keys = jax.random.split(jax.random.fold_in(key, 17), TOKENS // TOK_DEV)
    blocks = jax.vmap(route_block)(block_keys)
    return blocks.reshape(TOKENS, TOPK).astype(jnp.int32)


def with_spikes(array, key, source, target, shards_of, factor):
    owner, partner = [(jnp.arange(array.shape[axis_at]) // (array.shape[axis_at] // shards_of)).reshape([-1 if axis == axis_at else 1 for axis in range(array.ndim)]) for axis_at in (source, target)]
    chosen = jax.random.permutation(key, shards_of)[partner]
    strong = (owner == chosen) | (owner == (partner + shards_of // 2) % shards_of)
    return jnp.where(strong, factor * array, array)


def block_scale(stream_key, shape, shards, smallest, top_value):
    loudness = 1.0
    for position, parts in shards:
        heights = jax.random.uniform(jax.random.fold_in(jax.random.fold_in(stream_key, 6), position), (parts,), jnp.float32, smallest / len(shards), top_value / len(shards))
        loudness = loudness * jnp.repeat(jnp.exp(heights), shape[position] // parts).reshape((-1,) + (1,) * (len(shape) - 1 - position))
    return loudness


def gaussian(stream_key, extent, scale, bound, cuts=(), kind=jnp.bfloat16):
    entries = scale * jax.random.normal(stream_key, extent, jnp.float32)
    if cuts:
        entries = entries * block_scale(stream_key, extent, cuts, -0.22, 0.18)
    return jnp.clip(entries, -bound, bound).astype(kind)


def gaussian_with(key, dims, deviation, most, cuts, heavy, kind=jnp.bfloat16):
    result = deviation * jax.random.normal(key, dims, jnp.float32)
    if cuts:
        result = result * block_scale(key, dims, cuts, -0.22, 0.18)
    return jnp.clip(with_spikes(result, jax.random.fold_in(key, 3), *heavy), -most, most).astype(kind)


def setup_inputs(seed: int = 0) -> dict:
    key_list = jax.random.split(jax.random.key(seed), 13)
    return {
        "moe_in": gaussian(key_list[0], (TOKENS, D), 1.0, 6.0, ((0, 8),)),
        "cotangent": gaussian_with(key_list[1], (TOKENS, D), 1.0, 6.0, ((0, 8),), (0, 1, 8, 2.0)),
        "routing": draw_routing(jax.random.fold_in(key_list[12], 71), 0),
        "route_weight": jnp.clip(0.2 + 0.8 * jax.random.uniform(key_list[3], (TOKENS, TOPK), jnp.float32) ** block_scale(key_list[3], (TOKENS, TOPK), ((0, 8),), -0.2, 0.2), 0.2, 1.0),
        "w_gate": gaussian(key_list[4], (EXPERTS, HID, D), D ** -0.5, 0.125, ((0, 8), (1, 4))),
        "w_up": gaussian(key_list[5], (EXPERTS, HID, D), D ** -0.5, 0.125, ((0, 8), (1, 4))),
        "w_down": gaussian(key_list[6], (EXPERTS, HID, D), HID ** -0.5, 0.125, ((0, 8), (1, 4))),
        "gate_b": gaussian(key_list[7], (W_A, TOKENS), 1.0, 6.0, ((0, 4), (1, 8))),
        "gate_c": gaussian(key_list[8], (W_A, TOKENS), 1.0, 6.0, ((0, 4), (1, 8))),
        "value_x": gaussian(key_list[9], (W_A, TOKENS), 1.0, 6.0, ((0, 4), (1, 8))),
        "conv_taps": gaussian(key_list[10], (TAPS, W_A), 0.6, 3.0, ((1, 4),), jnp.float32),
        "out_proj": gaussian(key_list[11], (W_A, D), W_A ** -0.5, 0.1875, ((0, 4),)),
    }


def reference(moe_in, cotangent, routing, route_weight, w_gate, w_up, w_down, gate_b, gate_c, value_x, conv_taps, out_proj):
    flat_routes = routing.reshape(-1)
    order = jnp.argsort(flat_routes, stable=True).astype(jnp.int32).reshape(EXPERTS, CAP * N_SP)
    weight_flat = route_weight.reshape(-1)
    contract_model = (((1,), (1,)), ((), ()))
    over_rows = (((0,), (0,)), ((), ()))

    def expert(packed):
        index, gate_weight, up_weight, down_weight = packed
        owner = index // TOPK
        arrived = moe_in[owner]
        route_cot = (weight_flat[index][:, None] * cotangent[owner].astype(jnp.float32)).astype(jnp.bfloat16)
        gate_pre = lax.dot_general(arrived, gate_weight, contract_model, preferred_element_type=jnp.float32)
        up_pre = lax.dot_general(arrived, up_weight, contract_model, preferred_element_type=jnp.float32)
        sigmoid_gate = jax.nn.sigmoid(gate_pre)
        hidden = (gate_pre * sigmoid_gate * up_pre).astype(jnp.bfloat16)
        hidden_grad = lax.dot_general(route_cot, down_weight, contract_model, preferred_element_type=jnp.float32)
        gate_grad = (hidden_grad * up_pre * sigmoid_gate * (1.0 + gate_pre * (1.0 - sigmoid_gate))).astype(jnp.bfloat16)
        up_grad = (hidden_grad * gate_pre * sigmoid_gate).astype(jnp.bfloat16)
        gate_wgrad = lax.dot_general(gate_grad, arrived, over_rows, preferred_element_type=jnp.float32).astype(jnp.bfloat16)
        up_wgrad = lax.dot_general(up_grad, arrived, over_rows, preferred_element_type=jnp.float32).astype(jnp.bfloat16)
        down_wgrad = lax.dot_general(hidden, route_cot, over_rows, preferred_element_type=jnp.float32).astype(jnp.bfloat16)
        row_total = gate_grad.shape[0]
        gate_blocks = gate_grad.astype(jnp.float32).reshape(row_total, N_TP, HID_DEV)
        up_blocks = up_grad.astype(jnp.float32).reshape(row_total, N_TP, HID_DEV)
        gate_table = gate_weight.astype(jnp.float32).reshape(N_TP, HID_DEV, D)
        up_table = up_weight.astype(jnp.float32).reshape(N_TP, HID_DEV, D)
        partial_value = jnp.einsum("rbh,bhd->brd", gate_blocks, gate_table) + jnp.einsum("rbh,bhd->brd", up_blocks, up_table)
        partial_value = lax.optimization_barrier(partial_value.astype(jnp.bfloat16)).astype(jnp.float32)
        route_grad = jnp.sum(partial_value, axis=0).astype(jnp.bfloat16)
        return gate_wgrad, up_wgrad, down_wgrad, route_grad

    w_gate_grad, w_up_grad, w_down_grad, route_grads = lax.map(expert, (order, w_gate, w_up, w_down))
    placed = jnp.zeros((TOKENS * TOPK, D), jnp.float32).at[order.reshape(-1)].set(route_grads.reshape(-1, D).astype(jnp.float32))
    moe_in_grad = jnp.sum(placed.reshape(TOKENS, TOPK, D), axis=1).astype(jnp.bfloat16)

    stream_grad = (cotangent.astype(jnp.float32) + moe_in_grad.astype(jnp.float32)).astype(jnp.bfloat16)
    mixed_in = lax.optimization_barrier((gate_c.astype(jnp.float32) * value_x.astype(jnp.float32)).astype(jnp.bfloat16))
    extended = jnp.pad(mixed_in.astype(jnp.float32), ((0, 0), (TAPS - 1, 0)))
    conv_out = jnp.zeros((W_A, TOKENS), jnp.float32)
    for tap in range(TAPS):
        conv_out = conv_out + conv_taps[tap][:, None] * extended[:, tap:tap + TOKENS]
    mixer_act = (gate_b.astype(jnp.float32) * conv_out).astype(jnp.bfloat16)
    act_grad = lax.dot_general(out_proj, stream_grad, contract_model, preferred_element_type=jnp.float32)
    proj_grad = jnp.dot(mixer_act, stream_grad, preferred_element_type=jnp.float32)
    gate_b_grad = (act_grad * conv_out).astype(jnp.bfloat16)
    conv_grad = act_grad * gate_b.astype(jnp.float32)
    extended_grad = jnp.pad(conv_grad, ((0, 0), (0, TAPS - 1)))
    mixed_grad = jnp.zeros((W_A, TOKENS), jnp.float32)
    for tap in range(TAPS):
        offset = TAPS - 1 - tap
        mixed_grad = mixed_grad + conv_taps[tap][:, None] * extended_grad[:, offset:offset + TOKENS]
    gate_c_grad = (mixed_grad * value_x.astype(jnp.float32)).astype(jnp.bfloat16)
    value_x_grad = (mixed_grad * gate_c.astype(jnp.float32)).astype(jnp.bfloat16)
    return (w_gate_grad, w_up_grad, w_down_grad, moe_in_grad, proj_grad, gate_b_grad, gate_c_grad, value_x_grad)
```

```python
import jax
import jax.numpy as jnp
from jax import lax
from jax.experimental import pallas as pl
from jax.experimental.pallas import tpu as pltpu
from jax.sharding import PartitionSpec as P

TAPS = 3
GROUPS = 4
CORES = 2
MESH = pl.DeviceIdType.MESH


def place():
    s, t = lax.axis_index("sp"), lax.axis_index("tp")
    z, c = lax.div(s, CORES), lax.rem(s, CORES)
    x, y = lax.rem(t, 2), lax.div(t, 2)
    lanes = (t + 1 - 2 * x, t + 2 - 4 * y, 3 - t)
    return s, t, z, c, lanes


def greet(targets):
    barrier = pltpu.get_barrier_semaphore()
    for target in targets:
        pl.semaphore_signal(barrier, inc=1, device_id=target, device_id_type=MESH)
    pl.semaphore_wait(barrier, len(targets))


def span(index, width):
    return pl.ds(pl.multiple_of(index * width, width), width)


def remote(src, dst, send_sem, recv_sem, target):
    return pltpu.make_async_remote_copy(
        src_ref=src,
        dst_ref=dst,
        send_sem=send_sem,
        recv_sem=recv_sem,
        device_id=target,
        device_id_type=MESH,
    )


def dispatch_kernel(
    rows_ref, weight_ref, out_ref, weight_out, s1, r1, s2, r2, s3, r3, sw, rw, sp_, rp_, own
):
    s, t, z, c, lanes = place()
    width = rows_ref.shape[-1] // 4
    mate = (CORES * z + 1 - c, t)
    ahead = [lax.rem(z + d, GROUPS) for d in range(GROUPS)]
    behind = [lax.rem(z + GROUPS - d, GROUPS) for d in range(GROUPS)]
    greet(
        [(CORES * ahead[d] + c, t) for d in range(1, GROUPS)]
        + [(CORES * ahead[d] + 1 - c, t) for d in range(1, GROUPS)]
        + [(s, lanes[0]), (s, lanes[1]), mate]
    )
    quarters = (t, lanes[2])
    first = {}
    small = []
    for d in (2, 1, 3):
        for j in range(2):
            cols = span(quarters[j], width)
            copy = remote(
                rows_ref.at[ahead[d], :, :, cols],
                out_ref.at[:, s, :, cols],
                s1.at[j, d - 1],
                r1.at[j, d - 1],
                (CORES * ahead[d] + c, t),
            )
            copy.start()
            first[j, d] = copy
        for k in range(2):
            core = c if k == 0 else 1 - c
            copy = remote(
                weight_ref.at[ahead[d]],
                weight_out.at[s],
                sw.at[k, d - 1],
                rw.at[k, d - 1],
                (CORES * ahead[d] + core, t),
            )
            copy.start()
            small.append(copy)
    pair = [
        remote(rows_ref.at[z], out_ref.at[:, s], sp_.at[0], rp_.at[0], mate),
        remote(weight_ref.at[z], weight_out.at[s], sp_.at[1], rp_.at[1], mate),
    ]
    local = [
        pltpu.make_async_copy(rows_ref.at[z], out_ref.at[:, s], own.at[0]),
        pltpu.make_async_copy(weight_ref.at[z], weight_out.at[s], own.at[1]),
    ]
    for copy in pair + local:
        copy.start()
    order = (1, 3, 2)
    second = {}
    for d in order:
        first[0, d].wait_recv()
        cols = span(t, width)
        block = out_ref.at[:, CORES * behind[d] + c, :, cols]
        for j in range(2):
            copy = remote(block, block, s2.at[j, d - 1], r2.at[j, d - 1], (s, lanes[j]))
            copy.start()
            second[j, d] = copy
    third = []
    for d in order:
        first[1, d].wait_recv()
        second[0, d].wait_recv()
        second[1, d].wait_recv()
        block = out_ref.at[:, CORES * behind[d] + c]
        copy = remote(block, block, s3.at[d - 1], r3.at[d - 1], mate)
        copy.start()
        third.append(copy)
    for copy in local:
        copy.wait()
    for copy in small + pair + third:
        copy.wait()
    for copy in list(first.values()) + list(second.values()):
        copy.wait_send()


def dispatch(rows, weights):
    groups, two, cap, model = rows.shape
    vmem = pl.BlockSpec(memory_space=pltpu.VMEM)
    dma = pltpu.SemaphoreType.DMA
    return pl.pallas_call(
        dispatch_kernel,
        out_shape=(
            jax.ShapeDtypeStruct((two, CORES * groups, cap, model), rows.dtype),
            jax.ShapeDtypeStruct((CORES * groups,) + weights.shape[1:], weights.dtype),
        ),
        in_specs=[vmem, vmem],
        out_specs=(vmem, vmem),
        scratch_shapes=[
            dma((2, groups - 1)),
            dma((2, groups - 1)),
            dma((2, groups - 1)),
            dma((2, groups - 1)),
            dma((groups - 1,)),
            dma((groups - 1,)),
            dma((2, groups - 1)),
            dma((2, groups - 1)),
            dma((2,)),
            dma((2,)),
            dma((2,)),
        ],
        compiler_params=pltpu.CompilerParams(collective_id=0, has_side_effects=True),
        name="dispatch",
    )(rows, weights)


def combine_kernel(part_ref, out_ref, mate_in, total, lane_in, done, sa, ra, sb, rb, sc, rc, sd, rd):
    s, t, z, c, lanes = place()
    width = part_ref.shape[-1] // 4
    mate = (CORES * z + 1 - c, t)
    ahead = [lax.rem(z + d, GROUPS) for d in range(GROUPS)]
    behind = [lax.rem(z + GROUPS - d, GROUPS) for d in range(GROUPS)]
    greet(
        [(CORES * ahead[d] + c, t) for d in range(1, GROUPS)]
        + [(s, lane) for lane in lanes]
        + [mate]
    )
    order = (2, 1, 3, 0)
    mine = span(t, width)
    swap = {}
    for d in order:
        swap[d] = remote(part_ref.at[ahead[d], 1 - c], mate_in.at[d], sa.at[d], ra.at[d], mate)
        swap[d].start()
    across = {}
    for d in order:
        swap[d].wait_recv()
        total[d] = (
            part_ref[ahead[d], c].astype(jnp.float32) + mate_in[d].astype(jnp.float32)
        ).astype(total.dtype)
        for j in (2, 0, 1):
            across[j, d] = remote(
                total.at[d, :, span(lanes[j], width)],
                lane_in.at[j, d],
                sb.at[j, d],
                rb.at[j, d],
                (s, lanes[j]),
            )
            across[j, d].start()
    home = {}
    for d in order:
        value = total[d, :, mine].astype(jnp.float32)
        for j in range(3):
            across[j, d].wait_recv()
            value = value + lane_in[j, d].astype(jnp.float32)
        value = value.astype(out_ref.dtype)
        if d == 0:
            out_ref[z, :, mine] = value
        else:
            done[d - 1] = value
            home[d] = remote(
                done.at[d - 1],
                out_ref.at[z, :, mine],
                sc.at[d - 1],
                rc.at[d - 1],
                (CORES * ahead[d] + c, t),
            )
            home[d].start()
    spread = []
    for d in (0, 1, 3, 2):
        if d:
            home[d].wait_recv()
        block = out_ref.at[behind[d], :, mine]
        for j in (2, 0, 1):
            copy = remote(block, block, sd.at[j, d], rd.at[j, d], (s, lanes[j]))
            copy.start()
            spread.append(copy)
    for copy in spread:
        copy.wait()
    for copy in list(swap.values()) + list(across.values()) + list(home.values()):
        copy.wait_send()


def combine(part):
    groups, cores, cap, model = part.shape
    vmem = pl.BlockSpec(memory_space=pltpu.VMEM)
    dma = pltpu.SemaphoreType.DMA
    width = model // 4
    return pl.pallas_call(
        combine_kernel,
        out_shape=jax.ShapeDtypeStruct((groups, cap, model), part.dtype),
        in_specs=[vmem],
        out_specs=vmem,
        scratch_shapes=[
            pltpu.VMEM((groups, cap, model), part.dtype),
            pltpu.VMEM((groups, cap, model), part.dtype),
            pltpu.VMEM((3, groups, cap, width), part.dtype),
            pltpu.VMEM((groups - 1, cap, width), part.dtype),
            dma((groups,)),
            dma((groups,)),
            dma((3, groups)),
            dma((3, groups)),
            dma((groups - 1,)),
            dma((groups - 1,)),
            dma((3, groups)),
            dma((3, groups)),
        ],
        compiler_params=pltpu.CompilerParams(collective_id=1, has_side_effects=True),
        name="combine",
    )(part)


def project_kernel(part_ref, out_ref, mate_in, total, far_in, sa, ra, sb, rb):
    s, t, z, c, lanes = place()
    width = out_ref.shape[1]
    mate = (CORES * z + 1 - c, t)
    ahead = [lax.rem(z + d, GROUPS) for d in range(GROUPS)]
    greet([(CORES * ahead[d] + c, t) for d in range(1, GROUPS)] + [mate])
    order = (2, 1, 3, 0)
    swap = {}
    for d in order:
        cols = span(CORES * ahead[d] + 1 - c, width)
        swap[d] = remote(part_ref.at[:, cols], mate_in.at[d], sa.at[d], ra.at[d], mate)
        swap[d].start()
    far = {}
    for d in order:
        swap[d].wait_recv()
        cols = span(CORES * ahead[d] + c, width)
        value = part_ref[:, cols].astype(jnp.float32) + mate_in[d].astype(jnp.float32)
        if d == 0:
            out_ref[...] = value
        else:
            total[d - 1] = value.astype(total.dtype)
            far[d] = remote(
                total.at[d - 1],
                far_in.at[d - 1],
                sb.at[d - 1],
                rb.at[d - 1],
                (CORES * ahead[d] + c, t),
            )
            far[d].start()
    for d in range(1, GROUPS):
        far[d].wait_recv()
    out_ref[...] += (
        far_in[0].astype(jnp.float32) + far_in[1].astype(jnp.float32)
    ) + far_in[2].astype(jnp.float32)
    for copy in list(swap.values()) + list(far.values()):
        copy.wait_send()


def project(part):
    channels, model = part.shape
    width = model // (CORES * GROUPS)
    vmem = pl.BlockSpec(memory_space=pltpu.VMEM)
    dma = pltpu.SemaphoreType.DMA
    return pl.pallas_call(
        project_kernel,
        out_shape=jax.ShapeDtypeStruct((channels, width), jnp.float32),
        in_specs=[vmem],
        out_specs=vmem,
        scratch_shapes=[
            pltpu.VMEM((GROUPS, channels, width), part.dtype),
            pltpu.VMEM((GROUPS - 1, channels, width), part.dtype),
            pltpu.VMEM((GROUPS - 1, channels, width), part.dtype),
            dma((GROUPS,)),
            dma((GROUPS,)),
            dma((GROUPS - 1,)),
            dma((GROUPS - 1,)),
        ],
        compiler_params=pltpu.CompilerParams(collective_id=2, has_side_effects=True),
        name="project",
    )(part)


def from_behind(array, axis, by):
    count = lax.axis_size(axis)
    pairs = [(i, i + by) for i in range(count) if 0 <= i + by < count]
    return lax.ppermute(array, axis, pairs)


def on_device_general(
    moe_in,
    cotangent,
    routing,
    route_weight,
    w_gate,
    w_up,
    w_down,
    gate_b,
    gate_c,
    value_x,
    conv_taps,
    out_proj,
):
    tok_rows = routing.shape[0]
    top_routes = routing.shape[1]
    experts = lax.axis_size("sp")
    lane_count = lax.axis_size("tp")
    model_width = moe_in.shape[1]
    capacity = top_routes * tok_rows // experts
    flat_routes = routing.reshape(-1)
    route_count = flat_routes.shape[0]
    one_hot = (flat_routes[:, None] == jnp.arange(experts, dtype=jnp.int32)[None, :]).astype(
        jnp.int32
    )
    slot_rank = jnp.sum(jnp.cumsum(one_hot, axis=0) * one_hot, axis=1) - 1
    slot_index = flat_routes * capacity + slot_rank
    source = (
        jnp.zeros((route_count,), jnp.int32)
        .at[slot_index]
        .set(jnp.arange(route_count, dtype=jnp.int32))
    )
    owner_token = source // top_routes
    scales = route_weight.reshape(-1)[source][:, None]
    col_width = model_width // lane_count
    col_start = lax.axis_index("tp") * col_width
    rows_part = lax.dynamic_slice_in_dim(moe_in, col_start, col_width, 1)[owner_token]
    cot_slice = lax.dynamic_slice_in_dim(cotangent, col_start, col_width, 1)[owner_token]
    cot_part = (scales * cot_slice.astype(jnp.float32)).astype(jnp.bfloat16)
    moved = (
        lax.all_to_all(rows_part, "sp", split_axis=0, concat_axis=0, tiled=True),
        lax.all_to_all(cot_part, "sp", split_axis=0, concat_axis=0, tiled=True),
    )
    arrived, arrived_cot = (
        lax.all_gather(moved[0], "tp", axis=1, tiled=True),
        lax.all_gather(moved[1], "tp", axis=1, tiled=True),
    )
    contract_model = (((1,), (1,)), ((), ()))
    over_rows = (((0,), (0,)), ((), ()))
    gate_pre = lax.dot_general(
        arrived, w_gate[0], contract_model, preferred_element_type=jnp.float32
    )
    up_pre = lax.dot_general(arrived, w_up[0], contract_model, preferred_element_type=jnp.float32)
    sigmoid_gate = jax.nn.sigmoid(gate_pre)
    hidden = (gate_pre * sigmoid_gate * up_pre).astype(jnp.bfloat16)
    hidden_grad = lax.dot_general(
        arrived_cot, w_down[0], contract_model, preferred_element_type=jnp.float32
    )
    gate_grad = (
        hidden_grad * up_pre * sigmoid_gate * (1.0 + gate_pre * (1.0 - sigmoid_gate))
    ).astype(jnp.bfloat16)
    up_grad = (hidden_grad * gate_pre * sigmoid_gate).astype(jnp.bfloat16)
    w_gate_grad = lax.dot_general(
        gate_grad, arrived, over_rows, preferred_element_type=jnp.float32
    ).astype(jnp.bfloat16)[None]
    w_up_grad = lax.dot_general(
        up_grad, arrived, over_rows, preferred_element_type=jnp.float32
    ).astype(jnp.bfloat16)[None]
    w_down_grad = lax.dot_general(
        hidden, arrived_cot, over_rows, preferred_element_type=jnp.float32
    ).astype(jnp.bfloat16)[None]
    partial_value = jnp.dot(gate_grad, w_gate[0], preferred_element_type=jnp.float32) + jnp.dot(
        up_grad, w_up[0], preferred_element_type=jnp.float32
    )
    partial_value = lax.optimization_barrier(partial_value.astype(jnp.bfloat16)).astype(jnp.float32)
    summed = lax.psum_scatter(
        partial_value.astype(jnp.bfloat16), "tp", scatter_dimension=1, tiled=True
    )
    returned = lax.all_to_all(summed, "sp", split_axis=0, concat_axis=0, tiled=True)
    per_route = returned[slot_index].astype(jnp.float32)
    moe_in_grad = jnp.sum(per_route.reshape(tok_rows, top_routes, -1), axis=1).astype(jnp.bfloat16)
    full_grad = lax.all_gather(moe_in_grad, "tp", axis=1, tiled=True)
    stream_grad = (cotangent.astype(jnp.float32) + full_grad.astype(jnp.float32)).astype(
        jnp.bfloat16
    )
    mixed_in = lax.optimization_barrier(
        (gate_c.astype(jnp.float32) * value_x.astype(jnp.float32)).astype(jnp.bfloat16)
    )
    earlier = from_behind(mixed_in[:, tok_rows - (TAPS - 1) :], "sp", 1)
    extended = jnp.concatenate([earlier, mixed_in], axis=1).astype(jnp.float32)
    conv_out = jnp.zeros(mixed_in.shape, jnp.float32)
    for tap in range(TAPS):
        conv_out = conv_out + conv_taps[tap][:, None] * extended[:, tap : tap + tok_rows]
    mixer_act = (gate_b.astype(jnp.float32) * conv_out).astype(jnp.bfloat16)
    act_grad = lax.dot_general(
        out_proj, stream_grad, contract_model, preferred_element_type=jnp.float32
    )
    proj_rows = lax.psum_scatter(
        lax.dot_general(
            stream_grad, mixer_act, (((0,), (1,)), ((), ())), preferred_element_type=jnp.float32
        ).astype(jnp.bfloat16),
        "sp",
        scatter_dimension=0,
        tiled=True,
    ).astype(jnp.float32)
    proj_grad = proj_rows.T
    gate_b_grad = (act_grad * conv_out).astype(jnp.bfloat16)
    conv_grad = act_grad * gate_b.astype(jnp.float32)
    later = from_behind(conv_grad[:, : TAPS - 1], "sp", -1)
    extended_grad = jnp.concatenate([conv_grad, later], axis=1)
    mixed_grad = jnp.zeros(conv_grad.shape, jnp.float32)
    for tap in range(TAPS):
        offset = TAPS - 1 - tap
        mixed_grad = (
            mixed_grad + conv_taps[tap][:, None] * extended_grad[:, offset : offset + tok_rows]
        )
    gate_c_grad = (mixed_grad * value_x.astype(jnp.float32)).astype(jnp.bfloat16)
    value_x_grad = (mixed_grad * gate_c.astype(jnp.float32)).astype(jnp.bfloat16)
    return (
        w_gate_grad,
        w_up_grad,
        w_down_grad,
        moe_in_grad,
        proj_grad,
        gate_b_grad,
        gate_c_grad,
        value_x_grad,
    )


def on_device_paired(
    moe_in,
    cotangent,
    routing,
    route_weight,
    w_gate,
    w_up,
    w_down,
    gate_b,
    gate_c,
    value_x,
    conv_taps,
    out_proj,
):
    tok_rows = routing.shape[0]
    lane_count = lax.axis_size("tp")
    model_width = moe_in.shape[1]
    cap = tok_rows // GROUPS
    core = lax.rem(lax.axis_index("sp"), CORES)
    group = routing[:, 0] // CORES
    at = jnp.arange(tok_rows, dtype=jnp.int32)
    same = (group[:, None] == group[None, :]) & (at[:, None] < at[None, :])
    position = group * cap + jnp.sum(same.astype(jnp.int32), axis=0)
    select = position[None, :] == at[:, None]
    permute = select.astype(jnp.bfloat16)
    is_even = routing[:, 0] % CORES == 0
    by_core = jnp.stack(
        [
            jnp.where(is_even, route_weight[:, 0], route_weight[:, 1]),
            jnp.where(is_even, route_weight[:, 1], route_weight[:, 0]),
        ]
    )
    weights = jnp.sum(jnp.where(select[None], by_core[:, None, :], 0.0), axis=2)
    weights = weights.reshape(CORES, GROUPS, cap).transpose(1, 0, 2)
    weights = jnp.pad(weights, ((0, 0), (0, 8 - CORES), (0, 128 - cap)))
    rows = jnp.stack(
        [
            jnp.dot(permute, array, preferred_element_type=jnp.float32)
            .astype(jnp.bfloat16)
            .reshape(GROUPS, cap, model_width)
            for array in (moe_in, cotangent)
        ],
        axis=1,
    )
    landed, landed_weights = dispatch(rows, weights)
    arrived = landed[0].reshape(-1, model_width)
    scales = lax.dynamic_index_in_dim(landed_weights, core, 1, False)[:, :cap].reshape(-1, 1)
    arrived_cot = (scales * landed[1].reshape(-1, model_width).astype(jnp.float32)).astype(
        jnp.bfloat16
    )
    contract_model = (((1,), (1,)), ((), ()))
    over_rows = (((0,), (0,)), ((), ()))
    gate_pre = lax.dot_general(
        arrived, w_gate[0], contract_model, preferred_element_type=jnp.float32
    )
    up_pre = lax.dot_general(arrived, w_up[0], contract_model, preferred_element_type=jnp.float32)
    sigmoid_gate = jax.nn.sigmoid(gate_pre)
    hidden = (gate_pre * sigmoid_gate * up_pre).astype(jnp.bfloat16)
    hidden_grad = lax.dot_general(
        arrived_cot, w_down[0], contract_model, preferred_element_type=jnp.float32
    )
    gate_grad = (
        hidden_grad * up_pre * sigmoid_gate * (1.0 + gate_pre * (1.0 - sigmoid_gate))
    ).astype(jnp.bfloat16)
    up_grad = (hidden_grad * gate_pre * sigmoid_gate).astype(jnp.bfloat16)
    w_gate_grad = lax.dot_general(
        gate_grad, arrived, over_rows, preferred_element_type=jnp.float32
    ).astype(jnp.bfloat16)[None]
    w_up_grad = lax.dot_general(
        up_grad, arrived, over_rows, preferred_element_type=jnp.float32
    ).astype(jnp.bfloat16)[None]
    w_down_grad = lax.dot_general(
        hidden, arrived_cot, over_rows, preferred_element_type=jnp.float32
    ).astype(jnp.bfloat16)[None]
    partial_value = jnp.dot(gate_grad, w_gate[0], preferred_element_type=jnp.float32) + jnp.dot(
        up_grad, w_up[0], preferred_element_type=jnp.float32
    )
    summed = combine(
        partial_value.astype(jnp.bfloat16).reshape(GROUPS, CORES, cap, model_width)
    )
    full_grad = lax.dot_general(
        permute,
        summed.reshape(tok_rows, model_width),
        over_rows,
        preferred_element_type=jnp.float32,
    ).astype(jnp.bfloat16)
    col_width = model_width // lane_count
    moe_in_grad = lax.dynamic_slice_in_dim(
        full_grad, lax.axis_index("tp") * col_width, col_width, 1
    )
    stream_grad = (cotangent.astype(jnp.float32) + full_grad.astype(jnp.float32)).astype(
        jnp.bfloat16
    )
    mixed_in = lax.optimization_barrier(
        (gate_c.astype(jnp.float32) * value_x.astype(jnp.float32)).astype(jnp.bfloat16)
    )
    earlier = from_behind(mixed_in[:, tok_rows - (TAPS - 1) :], "sp", 1)
    extended = jnp.concatenate([earlier, mixed_in], axis=1).astype(jnp.float32)
    conv_out = jnp.zeros(mixed_in.shape, jnp.float32)
    for tap in range(TAPS):
        conv_out = conv_out + conv_taps[tap][:, None] * extended[:, tap : tap + tok_rows]
    mixer_act = (gate_b.astype(jnp.float32) * conv_out).astype(jnp.bfloat16)
    act_grad = lax.dot_general(
        out_proj, stream_grad, contract_model, preferred_element_type=jnp.float32
    )
    proj_grad = project(
        jnp.dot(mixer_act, stream_grad, preferred_element_type=jnp.float32).astype(jnp.bfloat16)
    )
    gate_b_grad = (act_grad * conv_out).astype(jnp.bfloat16)
    conv_grad = act_grad * gate_b.astype(jnp.float32)
    later = from_behind(conv_grad[:, : TAPS - 1], "sp", -1)
    extended_grad = jnp.concatenate([conv_grad, later], axis=1)
    mixed_grad = jnp.zeros(conv_grad.shape, jnp.float32)
    for tap in range(TAPS):
        offset = TAPS - 1 - tap
        mixed_grad = (
            mixed_grad + conv_taps[tap][:, None] * extended_grad[:, offset : offset + tok_rows]
        )
    gate_c_grad = (mixed_grad * value_x.astype(jnp.float32)).astype(jnp.bfloat16)
    value_x_grad = (mixed_grad * gate_c.astype(jnp.float32)).astype(jnp.bfloat16)
    return (
        w_gate_grad,
        w_up_grad,
        w_down_grad,
        moe_in_grad,
        proj_grad,
        gate_b_grad,
        gate_c_grad,
        value_x_grad,
    )


def on_device(*args):
    routes = args[2].shape[1]
    experts, lane_count = lax.axis_size("sp"), lax.axis_size("tp")
    if experts == CORES * GROUPS and routes == CORES and lane_count == 4:
        return on_device_paired(*args)
    return on_device_general(*args)


def solution(mesh):
    in_specs = (
        P("sp", None),
        P("sp", None),
        P("sp", None),
        P("sp", None),
        P("sp", "tp", None),
        P("sp", "tp", None),
        P("sp", "tp", None),
        P("tp", "sp"),
        P("tp", "sp"),
        P("tp", "sp"),
        P(None, "tp"),
        P("tp", None),
    )
    out_specs = (
        P("sp", "tp", None),
        P("sp", "tp", None),
        P("sp", "tp", None),
        P("sp", "tp"),
        P("tp", "sp"),
        P("tp", "sp"),
        P("tp", "sp"),
        P("tp", "sp"),
    )
    return jax.shard_map(
        on_device, mesh=mesh, in_specs=in_specs, out_specs=out_specs, check_vma=False
    )
```

```python
import jax
import jax.numpy as jnp
from jax import lax
from jax.experimental import pallas as pl
from jax.experimental.pallas import tpu as pltpu
from jax.sharding import PartitionSpec as P

TAPS = 3
GROUPS = 4
CORES = 2
MESH = pl.DeviceIdType.MESH


def place():
    s, t = lax.axis_index("sp"), lax.axis_index("tp")
    z, c = lax.div(s, CORES), lax.rem(s, CORES)
    x, y = lax.rem(t, 2), lax.div(t, 2)
    lanes = (t + 1 - 2 * x, t + 2 - 4 * y, 3 - t)
    return s, t, z, c, lanes


def greet(targets):
    barrier = pltpu.get_barrier_semaphore()
    for target in targets:
        pl.semaphore_signal(barrier, inc=1, device_id=target, device_id_type=MESH)
    pl.semaphore_wait(barrier, len(targets))


def span(index, width):
    return pl.ds(pl.multiple_of(index * width, width), width)


def remote(src, dst, send_sem, recv_sem, target):
    return pltpu.make_async_remote_copy(
        src_ref=src,
        dst_ref=dst,
        send_sem=send_sem,
        recv_sem=recv_sem,
        device_id=target,
        device_id_type=MESH,
    )


def half(quarter, side, width):
    return pl.ds(pl.multiple_of(quarter * width + side * (width // 2), width // 2), width // 2)


def dispatch_kernel(
    position_ref,
    by_core_ref,
    moe_ref,
    cot_ref,
    out_x,
    out_cot,
    rows,
    weights,
    landed,
    weight_in,
    s1,
    r1,
    s2,
    r2,
    s3,
    r3,
    s4,
    r4,
    sw,
    rw,
    sm,
    rm,
    own,
):
    s, t, z, c, lanes = place()
    tokens, model = moe_ref.shape
    cap = tokens // GROUPS
    width = model // 4
    mate = (CORES * z + 1 - c, t)
    ahead = [lax.rem(z + d, GROUPS) for d in range(GROUPS)]
    behind = [lax.rem(z + GROUPS - d, GROUPS) for d in range(GROUPS)]
    targets = (
        [(CORES * ahead[d] + c, t) for d in range(1, GROUPS)]
        + [(CORES * ahead[d] + 1 - c, t) for d in range(1, GROUPS)]
        + [(s, lanes[0]), (s, lanes[1]), mate]
    )
    barrier = pltpu.get_barrier_semaphore()
    for target in targets:
        pl.semaphore_signal(barrier, inc=1, device_id=target, device_id_type=MESH)
    select = position_ref[...] == lax.broadcasted_iota(jnp.int32, (tokens, tokens), 0)
    permute = select.astype(jnp.float32).astype(jnp.bfloat16)
    rows[:, 0] = (
        jnp.dot(permute, moe_ref[...], preferred_element_type=jnp.float32)
        .astype(rows.dtype)
        .reshape(GROUPS, cap, model)
    )
    rows[:, 1] = (
        jnp.dot(permute, cot_ref[...], preferred_element_type=jnp.float32)
        .astype(rows.dtype)
        .reshape(GROUPS, cap, model)
    )
    columns = [
        jnp.sum(jnp.where(select, by_core_ref[k : k + 1, :], 0.0), axis=1, keepdims=True)
        for k in range(CORES)
    ]
    lane_at = lax.broadcasted_iota(jnp.int32, (tokens, 128), 1)
    weights[...] = jnp.where(lane_at == 0, columns[0], columns[1]).reshape(GROUPS, cap, 128)
    pl.semaphore_wait(barrier, len(targets))

    order = (2, 1, 3)
    mine = span(t, width)
    first = {}
    for d in order:
        first[d] = remote(
            rows.at[ahead[d], :, :, mine],
            landed.at[:, s, :, mine],
            s1.at[d - 1],
            r1.at[d - 1],
            (CORES * ahead[d] + c, t),
        )
        first[d].start()
    small = []
    for d in order:
        for k in range(2):
            core = c if k == 0 else 1 - c
            copy = remote(
                weights.at[ahead[d]],
                weight_in.at[s],
                sw.at[k, d - 1],
                rw.at[k, d - 1],
                (CORES * ahead[d] + core, t),
            )
            copy.start()
            small.append(copy)
    pair = [
        remote(rows.at[z], landed.at[:, s], sm.at[0], rm.at[0], mate),
        remote(weights.at[z], weight_in.at[s], sm.at[1], rm.at[1], mate),
    ]
    local = [
        pltpu.make_async_copy(rows.at[z], landed.at[:, s], own.at[0]),
        pltpu.make_async_copy(weights.at[z], weight_in.at[s], own.at[1]),
    ]
    for copy in pair + local:
        copy.start()

    def finish(source):
        at_core = lax.broadcasted_iota(jnp.int32, (cap, 128), 1) == c
        scale = jnp.sum(jnp.where(at_core, weight_in[source], 0.0), axis=1, keepdims=True)
        out_x[source] = landed[0, source]
        out_cot[source] = (scale * landed[1, source].astype(jnp.float32)).astype(out_cot.dtype)

    second = {}
    for d in order:
        first[d].wait_recv()
        block = landed.at[:, CORES * behind[d] + c, :, mine]
        for j in range(2):
            second[j, d] = remote(
                block, block, s2.at[j, d - 1], r2.at[j, d - 1], (s, lanes[j])
            )
            second[j, d].start()
    third = {}
    for d in order:
        for j in range(2):
            second[j, d].wait_recv()
        for j in range(2):
            block = landed.at[:, CORES * behind[d] + c, :, half(lanes[1 - j], j, width)]
            third[j, d] = remote(
                block, block, s3.at[j, d - 1], r3.at[j, d - 1], (s, lanes[j])
            )
            third[j, d].start()
    for copy in local:
        copy.wait()
    finish(s)
    for copy in pair:
        copy.wait()
    finish(CORES * z + 1 - c)
    for copy in small:
        copy.wait()
    fourth = {}
    for d in order:
        for j in range(2):
            third[j, d].wait_recv()
        block = landed.at[:, CORES * behind[d] + c]
        fourth[d] = remote(block, block, s4.at[d - 1], r4.at[d - 1], mate)
        fourth[d].start()
        finish(CORES * behind[d] + c)
    for d in order:
        fourth[d].wait_recv()
        finish(CORES * behind[d] + 1 - c)
    for group in (first, second, third, fourth):
        for copy in group.values():
            copy.wait_send()


def dispatch(position, by_core, moe_in, cotangent):
    tokens, model = moe_in.shape
    cap = tokens // GROUPS
    vmem = pl.BlockSpec(memory_space=pltpu.VMEM)
    dma = pltpu.SemaphoreType.DMA
    landing = jax.ShapeDtypeStruct((CORES * GROUPS, cap, model), moe_in.dtype)
    one, two = (GROUPS - 1,), (2, GROUPS - 1)
    return pl.pallas_call(
        dispatch_kernel,
        out_shape=(landing, landing),
        in_specs=[vmem] * 4,
        out_specs=(vmem, vmem),
        scratch_shapes=[
            pltpu.VMEM((GROUPS, 2, cap, model), moe_in.dtype),
            pltpu.VMEM((GROUPS, cap, 128), jnp.float32),
            pltpu.VMEM((2, CORES * GROUPS, cap, model), moe_in.dtype),
            pltpu.VMEM((CORES * GROUPS, cap, 128), jnp.float32),
        ]
        + [dma(one), dma(one)]
        + [dma(two) for _ in range(4)]
        + [dma(one), dma(one)]
        + [dma(two), dma(two)]
        + [dma((2,)) for _ in range(3)],
        compiler_params=pltpu.CompilerParams(collective_id=0, has_side_effects=True),
        name="dispatch",
    )(position, by_core, moe_in, cotangent)


def combine_kernel(part_ref, out_ref, mate_in, total, lane_in, done, sa, ra, sb, rb, sc, rc, sd, rd, se, re):
    s, t, z, c, lanes = place()
    width = part_ref.shape[-1] // 4
    mate = (CORES * z + 1 - c, t)
    ahead = [lax.rem(z + d, GROUPS) for d in range(GROUPS)]
    behind = [lax.rem(z + GROUPS - d, GROUPS) for d in range(GROUPS)]
    greet(
        [(CORES * ahead[d] + c, t) for d in range(1, GROUPS)]
        + [(s, lane) for lane in lanes]
        + [mate]
    )
    order = (2, 1, 3, 0)
    mine = span(t, width)
    swap = {}
    for d in order:
        swap[d] = remote(part_ref.at[ahead[d], 1 - c], mate_in.at[d], sa.at[d], ra.at[d], mate)
        swap[d].start()
    across = {}
    for d in order:
        swap[d].wait_recv()
        total[d] = (
            part_ref[ahead[d], c].astype(jnp.float32) + mate_in[d].astype(jnp.float32)
        ).astype(total.dtype)
        for j in (2, 0, 1):
            across[j, d] = remote(
                total.at[d, :, span(lanes[j], width)],
                lane_in.at[j, d],
                sb.at[j, d],
                rb.at[j, d],
                (s, lanes[j]),
            )
            across[j, d].start()
    home = {}
    for d in order:
        value = total[d, :, mine].astype(jnp.float32)
        for j in range(3):
            across[j, d].wait_recv()
            value = value + lane_in[j, d].astype(jnp.float32)
        value = value.astype(out_ref.dtype)
        if d == 0:
            out_ref[z, :, mine] = value
        else:
            done[d - 1] = value
            home[d] = remote(
                done.at[d - 1],
                out_ref.at[z, :, mine],
                sc.at[d - 1],
                rc.at[d - 1],
                (CORES * ahead[d] + c, t),
            )
            home[d].start()
    spread = {}
    for d in (0, 1, 3, 2):
        if d:
            home[d].wait_recv()
        block = out_ref.at[behind[d], :, mine]
        for j in range(2):
            spread[j, d] = remote(block, block, sd.at[j, d], rd.at[j, d], (s, lanes[j]))
            spread[j, d].start()
    relay = []
    for d in (0, 1, 3, 2):
        for j in range(2):
            spread[j, d].wait_recv()
        for j in range(2):
            block = out_ref.at[behind[d], :, half(lanes[1 - j], j, width)]
            copy = remote(block, block, se.at[j, d], re.at[j, d], (s, lanes[j]))
            copy.start()
            relay.append(copy)
    for copy in relay:
        copy.wait()
    for copy in spread.values():
        copy.wait_send()
    for copy in list(swap.values()) + list(across.values()) + list(home.values()):
        copy.wait_send()


def combine(part):
    groups, cores, cap, model = part.shape
    vmem = pl.BlockSpec(memory_space=pltpu.VMEM)
    dma = pltpu.SemaphoreType.DMA
    width = model // 4
    return pl.pallas_call(
        combine_kernel,
        out_shape=jax.ShapeDtypeStruct((groups, cap, model), part.dtype),
        in_specs=[vmem],
        out_specs=vmem,
        scratch_shapes=[
            pltpu.VMEM((groups, cap, model), part.dtype),
            pltpu.VMEM((groups, cap, model), part.dtype),
            pltpu.VMEM((3, groups, cap, width), part.dtype),
            pltpu.VMEM((groups - 1, cap, width), part.dtype),
            dma((groups,)),
            dma((groups,)),
            dma((3, groups)),
            dma((3, groups)),
            dma((groups - 1,)),
            dma((groups - 1,)),
            dma((2, groups)),
            dma((2, groups)),
            dma((2, groups)),
            dma((2, groups)),
        ],
        compiler_params=pltpu.CompilerParams(collective_id=1, has_side_effects=True),
        name="combine",
    )(part)


def project_kernel(part_ref, out_ref, far_in, mate_in, total, sa, ra, sb, rb):
    s, t, z, c, lanes = place()
    width = out_ref.shape[1]
    mate = (CORES * z + 1 - c, t)
    ahead = [lax.rem(z + d, GROUPS) for d in range(GROUPS)]
    greet([(CORES * ahead[d] + c, t) for d in range(1, GROUPS)] + [mate])
    order = (2, 1, 3, 0)
    swap = {}
    for d in order:
        cols = span(CORES * ahead[d] + 1 - c, width)
        swap[d] = remote(part_ref.at[:, cols], mate_in.at[d], sa.at[d], ra.at[d], mate)
        swap[d].start()
    far = {}
    for d in order:
        swap[d].wait_recv()
        cols = span(CORES * ahead[d] + c, width)
        value = part_ref[:, cols].astype(jnp.float32) + mate_in[d].astype(jnp.float32)
        if d == 0:
            out_ref[...] = value
        else:
            total[d - 1] = value.astype(total.dtype)
            far[d] = remote(
                total.at[d - 1],
                far_in.at[d - 1],
                sb.at[d - 1],
                rb.at[d - 1],
                (CORES * ahead[d] + c, t),
            )
            far[d].start()
    for d in range(1, GROUPS):
        far[d].wait_recv()
    for copy in list(swap.values()) + list(far.values()):
        copy.wait_send()


def project(part):
    channels, model = part.shape
    width = model // (CORES * GROUPS)
    vmem = pl.BlockSpec(memory_space=pltpu.VMEM)
    dma = pltpu.SemaphoreType.DMA
    return pl.pallas_call(
        project_kernel,
        out_shape=(
            jax.ShapeDtypeStruct((channels, width), jnp.float32),
            jax.ShapeDtypeStruct((GROUPS - 1, channels, width), part.dtype),
        ),
        in_specs=[vmem],
        out_specs=(vmem, vmem),
        scratch_shapes=[
            pltpu.VMEM((GROUPS, channels, width), part.dtype),
            pltpu.VMEM((GROUPS - 1, channels, width), part.dtype),
            dma((GROUPS,)),
            dma((GROUPS,)),
            dma((GROUPS - 1,)),
            dma((GROUPS - 1,)),
        ],
        compiler_params=pltpu.CompilerParams(collective_id=2, has_side_effects=True),
        name="project",
    )(part)


def from_behind(array, axis, by):
    count = lax.axis_size(axis)
    pairs = [(i, i + by) for i in range(count) if 0 <= i + by < count]
    return lax.ppermute(array, axis, pairs)


def on_device_general(
    moe_in,
    cotangent,
    routing,
    route_weight,
    w_gate,
    w_up,
    w_down,
    gate_b,
    gate_c,
    value_x,
    conv_taps,
    out_proj,
):
    tok_rows = routing.shape[0]
    top_routes = routing.shape[1]
    experts = lax.axis_size("sp")
    lane_count = lax.axis_size("tp")
    model_width = moe_in.shape[1]
    capacity = top_routes * tok_rows // experts
    flat_routes = routing.reshape(-1)
    route_count = flat_routes.shape[0]
    one_hot = (flat_routes[:, None] == jnp.arange(experts, dtype=jnp.int32)[None, :]).astype(
        jnp.int32
    )
    slot_rank = jnp.sum(jnp.cumsum(one_hot, axis=0) * one_hot, axis=1) - 1
    slot_index = flat_routes * capacity + slot_rank
    source = (
        jnp.zeros((route_count,), jnp.int32)
        .at[slot_index]
        .set(jnp.arange(route_count, dtype=jnp.int32))
    )
    owner_token = source // top_routes
    scales = route_weight.reshape(-1)[source][:, None]
    col_width = model_width // lane_count
    col_start = lax.axis_index("tp") * col_width
    rows_part = lax.dynamic_slice_in_dim(moe_in, col_start, col_width, 1)[owner_token]
    cot_slice = lax.dynamic_slice_in_dim(cotangent, col_start, col_width, 1)[owner_token]
    cot_part = (scales * cot_slice.astype(jnp.float32)).astype(jnp.bfloat16)
    moved = (
        lax.all_to_all(rows_part, "sp", split_axis=0, concat_axis=0, tiled=True),
        lax.all_to_all(cot_part, "sp", split_axis=0, concat_axis=0, tiled=True),
    )
    arrived, arrived_cot = (
        lax.all_gather(moved[0], "tp", axis=1, tiled=True),
        lax.all_gather(moved[1], "tp", axis=1, tiled=True),
    )
    contract_model = (((1,), (1,)), ((), ()))
    over_rows = (((0,), (0,)), ((), ()))
    gate_pre = lax.dot_general(
        arrived, w_gate[0], contract_model, preferred_element_type=jnp.float32
    )
    up_pre = lax.dot_general(arrived, w_up[0], contract_model, preferred_element_type=jnp.float32)
    sigmoid_gate = jax.nn.sigmoid(gate_pre)
    hidden = (gate_pre * sigmoid_gate * up_pre).astype(jnp.bfloat16)
    hidden_grad = lax.dot_general(
        arrived_cot, w_down[0], contract_model, preferred_element_type=jnp.float32
    )
    gate_grad = (
        hidden_grad * up_pre * sigmoid_gate * (1.0 + gate_pre * (1.0 - sigmoid_gate))
    ).astype(jnp.bfloat16)
    up_grad = (hidden_grad * gate_pre * sigmoid_gate).astype(jnp.bfloat16)
    w_gate_grad = lax.dot_general(
        gate_grad, arrived, over_rows, preferred_element_type=jnp.float32
    ).astype(jnp.bfloat16)[None]
    w_up_grad = lax.dot_general(
        up_grad, arrived, over_rows, preferred_element_type=jnp.float32
    ).astype(jnp.bfloat16)[None]
    w_down_grad = lax.dot_general(
        hidden, arrived_cot, over_rows, preferred_element_type=jnp.float32
    ).astype(jnp.bfloat16)[None]
    partial_value = jnp.dot(gate_grad, w_gate[0], preferred_element_type=jnp.float32) + jnp.dot(
        up_grad, w_up[0], preferred_element_type=jnp.float32
    )
    partial_value = lax.optimization_barrier(partial_value.astype(jnp.bfloat16)).astype(jnp.float32)
    summed = lax.psum_scatter(
        partial_value.astype(jnp.bfloat16), "tp", scatter_dimension=1, tiled=True
    )
    returned = lax.all_to_all(summed, "sp", split_axis=0, concat_axis=0, tiled=True)
    per_route = returned[slot_index].astype(jnp.float32)
    moe_in_grad = jnp.sum(per_route.reshape(tok_rows, top_routes, -1), axis=1).astype(jnp.bfloat16)
    full_grad = lax.all_gather(moe_in_grad, "tp", axis=1, tiled=True)
    stream_grad = (cotangent.astype(jnp.float32) + full_grad.astype(jnp.float32)).astype(
        jnp.bfloat16
    )
    mixed_in = lax.optimization_barrier(
        (gate_c.astype(jnp.float32) * value_x.astype(jnp.float32)).astype(jnp.bfloat16)
    )
    earlier = from_behind(mixed_in[:, tok_rows - (TAPS - 1) :], "sp", 1)
    extended = jnp.concatenate([earlier, mixed_in], axis=1).astype(jnp.float32)
    conv_out = jnp.zeros(mixed_in.shape, jnp.float32)
    for tap in range(TAPS):
        conv_out = conv_out + conv_taps[tap][:, None] * extended[:, tap : tap + tok_rows]
    mixer_act = (gate_b.astype(jnp.float32) * conv_out).astype(jnp.bfloat16)
    act_grad = lax.dot_general(
        out_proj, stream_grad, contract_model, preferred_element_type=jnp.float32
    )
    proj_rows = lax.psum_scatter(
        lax.dot_general(
            stream_grad, mixer_act, (((0,), (1,)), ((), ())), preferred_element_type=jnp.float32
        ).astype(jnp.bfloat16),
        "sp",
        scatter_dimension=0,
        tiled=True,
    ).astype(jnp.float32)
    proj_grad = proj_rows.T
    gate_b_grad = (act_grad * conv_out).astype(jnp.bfloat16)
    conv_grad = act_grad * gate_b.astype(jnp.float32)
    later = from_behind(conv_grad[:, : TAPS - 1], "sp", -1)
    extended_grad = jnp.concatenate([conv_grad, later], axis=1)
    mixed_grad = jnp.zeros(conv_grad.shape, jnp.float32)
    for tap in range(TAPS):
        offset = TAPS - 1 - tap
        mixed_grad = (
            mixed_grad + conv_taps[tap][:, None] * extended_grad[:, offset : offset + tok_rows]
        )
    gate_c_grad = (mixed_grad * value_x.astype(jnp.float32)).astype(jnp.bfloat16)
    value_x_grad = (mixed_grad * gate_c.astype(jnp.float32)).astype(jnp.bfloat16)
    return (
        w_gate_grad,
        w_up_grad,
        w_down_grad,
        moe_in_grad,
        proj_grad,
        gate_b_grad,
        gate_c_grad,
        value_x_grad,
    )


def on_device_paired(
    moe_in,
    cotangent,
    routing,
    route_weight,
    w_gate,
    w_up,
    w_down,
    gate_b,
    gate_c,
    value_x,
    conv_taps,
    out_proj,
):
    tok_rows = routing.shape[0]
    lane_count = lax.axis_size("tp")
    model_width = moe_in.shape[1]
    cap = tok_rows // GROUPS
    group = routing[:, 0] // CORES
    at = jnp.arange(tok_rows, dtype=jnp.int32)
    same = (group[:, None] == group[None, :]) & (at[:, None] < at[None, :])
    position = group * cap + jnp.sum(same.astype(jnp.int32), axis=0)
    select = position[None, :] == at[:, None]
    permute = select.astype(jnp.bfloat16)
    is_even = routing[:, 0] % CORES == 0
    by_core = jnp.stack(
        [
            jnp.where(is_even, route_weight[:, 0], route_weight[:, 1]),
            jnp.where(is_even, route_weight[:, 1], route_weight[:, 0]),
        ]
    )
    landed, landed_cot = dispatch(position[None, :], by_core, moe_in, cotangent)
    arrived = landed.reshape(-1, model_width)
    arrived_cot = landed_cot.reshape(-1, model_width)
    contract_model = (((1,), (1,)), ((), ()))
    over_rows = (((0,), (0,)), ((), ()))
    gate_pre = lax.dot_general(
        arrived, w_gate[0], contract_model, preferred_element_type=jnp.float32
    )
    up_pre = lax.dot_general(arrived, w_up[0], contract_model, preferred_element_type=jnp.float32)
    sigmoid_gate = jax.nn.sigmoid(gate_pre)
    hidden = (gate_pre * sigmoid_gate * up_pre).astype(jnp.bfloat16)
    hidden_grad = lax.dot_general(
        arrived_cot, w_down[0], contract_model, preferred_element_type=jnp.float32
    )
    gate_grad = (
        hidden_grad * up_pre * sigmoid_gate * (1.0 + gate_pre * (1.0 - sigmoid_gate))
    ).astype(jnp.bfloat16)
    up_grad = (hidden_grad * gate_pre * sigmoid_gate).astype(jnp.bfloat16)
    w_gate_grad = lax.dot_general(
        gate_grad, arrived, over_rows, preferred_element_type=jnp.float32
    ).astype(jnp.bfloat16)[None]
    w_up_grad = lax.dot_general(
        up_grad, arrived, over_rows, preferred_element_type=jnp.float32
    ).astype(jnp.bfloat16)[None]
    w_down_grad = lax.dot_general(
        hidden, arrived_cot, over_rows, preferred_element_type=jnp.float32
    ).astype(jnp.bfloat16)[None]
    partial_value = jnp.dot(gate_grad, w_gate[0], preferred_element_type=jnp.float32) + jnp.dot(
        up_grad, w_up[0], preferred_element_type=jnp.float32
    )
    summed = combine(
        partial_value.astype(jnp.bfloat16).reshape(GROUPS, CORES, cap, model_width)
    )
    full_grad = lax.dot_general(
        permute,
        summed.reshape(tok_rows, model_width),
        over_rows,
        preferred_element_type=jnp.float32,
    ).astype(jnp.bfloat16)
    col_width = model_width // lane_count
    moe_in_grad = lax.dynamic_slice_in_dim(
        full_grad, lax.axis_index("tp") * col_width, col_width, 1
    )
    stream_grad = (cotangent.astype(jnp.float32) + full_grad.astype(jnp.float32)).astype(
        jnp.bfloat16
    )
    mixed_in = lax.optimization_barrier(
        (gate_c.astype(jnp.float32) * value_x.astype(jnp.float32)).astype(jnp.bfloat16)
    )
    earlier = from_behind(mixed_in[:, tok_rows - (TAPS - 1) :], "sp", 1)
    extended = jnp.concatenate([earlier, mixed_in], axis=1).astype(jnp.float32)
    conv_out = jnp.zeros(mixed_in.shape, jnp.float32)
    for tap in range(TAPS):
        conv_out = conv_out + conv_taps[tap][:, None] * extended[:, tap : tap + tok_rows]
    mixer_act = (gate_b.astype(jnp.float32) * conv_out).astype(jnp.bfloat16)
    act_grad = lax.dot_general(
        out_proj, stream_grad, contract_model, preferred_element_type=jnp.float32
    )
    near, far = project(
        jnp.dot(mixer_act, stream_grad, preferred_element_type=jnp.float32).astype(jnp.bfloat16)
    )
    proj_grad = near + jnp.sum(far.astype(jnp.float32), axis=0)
    gate_b_grad = (act_grad * conv_out).astype(jnp.bfloat16)
    conv_grad = act_grad * gate_b.astype(jnp.float32)
    later = from_behind(conv_grad[:, : TAPS - 1], "sp", -1)
    extended_grad = jnp.concatenate([conv_grad, later], axis=1)
    mixed_grad = jnp.zeros(conv_grad.shape, jnp.float32)
    for tap in range(TAPS):
        offset = TAPS - 1 - tap
        mixed_grad = (
            mixed_grad + conv_taps[tap][:, None] * extended_grad[:, offset : offset + tok_rows]
        )
    gate_c_grad = (mixed_grad * value_x.astype(jnp.float32)).astype(jnp.bfloat16)
    value_x_grad = (mixed_grad * gate_c.astype(jnp.float32)).astype(jnp.bfloat16)
    return (
        w_gate_grad,
        w_up_grad,
        w_down_grad,
        moe_in_grad,
        proj_grad,
        gate_b_grad,
        gate_c_grad,
        value_x_grad,
    )


def on_device(*args):
    routes = args[2].shape[1]
    experts, lane_count = lax.axis_size("sp"), lax.axis_size("tp")
    if experts == CORES * GROUPS and routes == CORES and lane_count == 4:
        return on_device_paired(*args)
    return on_device_general(*args)


def solution(mesh):
    in_specs = (
        P("sp", None),
        P("sp", None),
        P("sp", None),
        P("sp", None),
        P("sp", "tp", None),
        P("sp", "tp", None),
        P("sp", "tp", None),
        P("tp", "sp"),
        P("tp", "sp"),
        P("tp", "sp"),
        P(None, "tp"),
        P("tp", None),
    )
    out_specs = (
        P("sp", "tp", None),
        P("sp", "tp", None),
        P("sp", "tp", None),
        P("sp", "tp"),
        P("tp", "sp"),
        P("tp", "sp"),
        P("tp", "sp"),
        P("tp", "sp"),
    )
    return jax.shard_map(
        on_device, mesh=mesh, in_specs=in_specs, out_specs=out_specs, check_vma=False
    )
```
